32 devices in a mesh: sp: 8 (over z, y), dp: 4 (over x, core).
Axes of the slice: x: 2, y: 2, z: 4, core: 2. Of those that a mesh axis runs over, the one named last changes fastest.
Arguments:
- stream: bfloat16 [4, 1024, 2048], P('dp', 'sp'), may hold values from -1.796875 to 1.796875
- query_rows: bfloat16 [4, 1024, 2048], P('dp', 'sp'), may hold values from -5 to 5
- key_rows: bfloat16 [4, 1024, 2048], P('dp', 'sp'), may hold values from -5 to 5
- value_rows: bfloat16 [4, 1024, 2048], P('dp', 'sp'), may hold values from -6 to 6
- forget_sums: float32 [4, 16, 1024], P('dp', 'sp'), may hold values from -1024 to 0, as said below
- out_weight: bfloat16 [2048, 2048], replicated, may hold values from -1.5 to 1.5
- first_gain: float32 [2048], replicated, may hold values from 0.1 to 1.9
- expert_ids: int32 [4, 1024, 4], P('dp', 'sp'), may hold values from 0 to 31, all different within a row; in each aligned block of 128 rows (0 to 127, 128 to 255, ..., all dimensions but the last counted through in order) at most 24 rows name the same one
- route_scores: float32 [4, 1024, 4], P('dp', 'sp'), may hold values from -6 to 6
- gate_weight: bfloat16 [32, 2048, 512], P(('sp', 'dp')), may hold values from -0.5 to 0.5
- up_weight: bfloat16 [32, 2048, 512], P(('sp', 'dp')), may hold values from -0.5 to 0.5
- down_weight: bfloat16 [32, 512, 2048], P(('sp', 'dp')), may hold values from -0.0625 to 0.0625
- second_gain: float32 [2048], replicated, may hold values from 0.1 to 1.9
Outputs:
- mixed_stream: bfloat16 [4, 1024, 2048], P('dp', 'sp')
The draws below stay inside these ranges and needn't reach their ends.
Inputs may be any that keep to these rules, and one draw needn't show every extreme that they name: `expert_ids`: each row names 4 different experts; in the rows of one device no expert is named more than 24 times. `forget_sums`: along positions each head's values never rise.
All inputs are finite; a program needn't handle non-finite values.
Results may differ from the reference program's by a relative error of at most 0.0085.
Values may be sent and summed in bfloat16 or wider, within the bound.
A program may use at most 128 MiB of HBM per device.

```python
import math
import jax
import jax.numpy as jnp
import numpy as np
from jax import lax

D = 2048
HEAD_TOTAL = 16
HD = 128
FF = 512
TOP = 4
TOK_DEV = 128
SEQUENCE_LENGTH = 1024
SEQUENCE_COUNT = 4
EXPERTS = 32
CAP = 24


def draw_query_rows(key, part):
    bulk = jnp.clip(jax.random.normal(jax.random.fold_in(key, 1), (SEQUENCE_COUNT, SEQUENCE_LENGTH, HEAD_TOTAL * HD), jnp.float32), -4.0, 4.0)
    return bulk.astype(jnp.bfloat16)


def draw_key_rows(key, part):
    bulk = jnp.clip(jax.random.normal(jax.random.fold_in(key, 2), (SEQUENCE_COUNT, SEQUENCE_LENGTH, HEAD_TOTAL * HD), jnp.float32), -4.0, 4.0)
    return bulk.astype(jnp.bfloat16)


def draw_forget_sums(key, part):
    key_collection = jax.random.split(jax.random.fold_in(key, 3), 7)
    order = jax.random.permutation(key_collection[0], HEAD_TOTAL)
    fast_count = HEAD_TOTAL // 2
    slow_rate = 0.8 / SEQUENCE_LENGTH * jax.random.uniform(key_collection[1], (HEAD_TOTAL,), jnp.float32, 0.7, 1.4)
    fast_rate = jnp.exp(jax.random.uniform(key_collection[2], (HEAD_TOTAL,), jnp.float32, jnp.log(1.0 / 100.0), jnp.log(1.0 / 30.0)))
    decay_rates = jnp.where(order < fast_count, fast_rate, slow_rate)
    block_count = SEQUENCE_LENGTH // TOK_DEV
    scale_per_block = jnp.exp(jax.random.uniform(key_collection[3], (SEQUENCE_COUNT, 1, block_count), jnp.float32, jnp.log(0.5), jnp.log(2.0)))
    scale_per_block = jnp.repeat(scale_per_block, TOK_DEV, axis=2)
    coarse_estimate = jax.random.uniform(key_collection[4], (SEQUENCE_COUNT, HEAD_TOTAL, SEQUENCE_LENGTH), jnp.float32, 0.3, 1.7)
    surge_position = jax.random.randint(key_collection[5], (SEQUENCE_COUNT, HEAD_TOTAL, 2), 0, SEQUENCE_LENGTH)
    surge_length = jax.random.uniform(key_collection[6], (SEQUENCE_COUNT, HEAD_TOTAL, 2), jnp.float32, 0.22, 0.69)
    position_index = jnp.arange(SEQUENCE_LENGTH, dtype=jnp.int32)
    surge_events = jnp.sum(jnp.where(position_index[None, None, None, :] == surge_position[..., None], surge_length[..., None], 0.0), axis=2)
    gate_logarithms = -decay_rates[None, :, None] * scale_per_block * coarse_estimate - surge_events
    return jnp.cumsum(gate_logarithms, axis=2)


def block_scale(stream_key, extent, cuts, low, top_value):
    level, own = 1.0, jax.random.fold_in(stream_key, 6)
    for axis_at, parts in cuts:
        draws = jnp.exp(jax.random.uniform(jax.random.fold_in(own, axis_at), (parts,), jnp.float32, low / len(cuts), top_value / len(cuts)))
        level = level * jnp.repeat(draws, extent[axis_at] // parts).reshape([-1 if axis == axis_at else 1 for axis in range(len(extent))])
    return level


def routed_block(rng, own, number, rows, amount, top, limit, slope):
    order = jax.random.permutation(rng, amount)
    packed, usual = portions_of(amount, rows * top, limit, slope, True), portions_of(amount, rows * top, limit, slope, False)
    places = jnp.arange(amount)

    def named(tallies, turn):
        used = int((tallies > 0).sum())
        fixed = max(1, used // 4)
        passed = fixed + (places - fixed + turn * (used - fixed)) % max(1, amount - fixed)
        return jnp.zeros((amount,), jnp.int32).at[order[jnp.where(places < fixed, places, passed)]].set(jnp.asarray(tallies, jnp.int32))

    tallies = jnp.where(number % 4 == 0, named(packed, number // 4), named(usual, number - number // 4 - 1))
    mixed = jax.random.permutation(jax.random.fold_in(own, 3), amount)
    source_of, sink = mixed[0:amount // 2 * 2:2], mixed[1:amount // 2 * 2:2]
    slack = jnp.minimum(tallies[source_of] - 1, limit - tallies[sink]) // 2
    slack = jnp.where((source_of == order[0]) | (sink == order[0]) | (tallies[sink] == 0), 0, jnp.maximum(slack, 0))
    passed = jax.random.randint(jax.random.fold_in(own, 4), (amount // 2,), 0, 1 << 20) % (slack + 1)
    tallies = tallies.at[source_of].add(-passed).at[sink].add(passed)
    members = jnp.searchsorted(jnp.cumsum(tallies), jnp.arange(rows * top), side="right").astype(jnp.int32)
    listing = members.reshape(top, rows).T
    listing = listing[jax.random.permutation(jax.random.fold_in(own, 1), rows)]
    turn = jax.random.randint(jax.random.fold_in(own, 2), (rows, 1), 0, top)
    return jnp.take_along_axis(listing, (jnp.arange(top)[None, :] + turn) % top, axis=1)


def portions_of(amount, total, reach, lean, full):
    weights = [(1 << 20) // math.isqrt(grade ** lean) + 1 for grade in range(1, amount + 1)]
    largest = reach if full else min(reach, max(-(-total // amount), total * weights[0] // sum(weights)))
    least = 1 if total - largest >= amount - 1 else 0
    counts, spare = [largest] + [least] * (amount - 1), total - largest - least * (amount - 1)
    while spare > 0:
        movable = [i for i in range(1, amount) if counts[i] < largest] or [i for i in range(1, amount) if counts[i] < reach]
        whole, budget = sum([weights[i] for i in movable]), spare
        for i in movable:
            more = min(reach - counts[i], max(1, budget * weights[i] // whole), spare)
            counts[i] = counts[i] + more
            spare = spare - more
    return np.array(counts)


def bell_draw(own_key, dims, deviation, limit, cuts=(), held_as=jnp.bfloat16):
    entries = jax.random.normal(own_key, dims, jnp.float32) * deviation
    if len(cuts) > 0:
        entries = block_scale(own_key, dims, cuts, -0.22, 0.18) * entries
    return jnp.clip(entries, min=-limit, max=limit).astype(held_as)


def setup_inputs(seed: int = 0) -> dict:
    key_of = jax.random.split(jax.random.key(seed), 14)
    stream = bell_draw(key_of[0], (SEQUENCE_COUNT, SEQUENCE_LENGTH, D), 0.3, 1.796875, ((0, 4), (1, 8)))
    query_rows = draw_query_rows(jax.random.fold_in(key_of[13], 71), 0)
    key_rows = draw_key_rows(jax.random.fold_in(key_of[13], 71), 0)
    value_rows = bell_draw(key_of[3], (SEQUENCE_COUNT, SEQUENCE_LENGTH, HEAD_TOTAL * HD), 1.0, 6.0, ((0, 4), (1, 8)))
    forget_sums = draw_forget_sums(jax.random.fold_in(key_of[13], 71), 0)
    out_weight = bell_draw(key_of[5], (HEAD_TOTAL * HD, D), (HD // 8) ** -0.5, 1.5)
    first_gain = jnp.clip(1.0 + 0.18 * jax.random.normal(key_of[6], (D,), jnp.float32), 0.1, 1.9)
    expert_ids_keys = jax.random.split(jax.random.fold_in(key_of[7], 1), SEQUENCE_COUNT * SEQUENCE_LENGTH // TOK_DEV)
    expert_ids_turns = jax.random.permutation(jax.random.fold_in(key_of[7], 3), SEQUENCE_COUNT * SEQUENCE_LENGTH // TOK_DEV)
    expert_ids = jax.vmap(lambda own, number: routed_block(jax.random.fold_in(key_of[7], 2), own, number, TOK_DEV, EXPERTS, TOP, CAP, 2))(expert_ids_keys, expert_ids_turns).reshape((SEQUENCE_COUNT, SEQUENCE_LENGTH, TOP))
    route_scores = bell_draw(key_of[8], (SEQUENCE_COUNT, SEQUENCE_LENGTH, TOP), 1.0, 6.0, ((0, 4), (1, 8)), jnp.float32)
    gate_weight = bell_draw(key_of[9], (EXPERTS, D, FF), (D // 16) ** -0.5, 0.5, ((0, 32),))
    up_weight = bell_draw(key_of[10], (EXPERTS, D, FF), (D // 16) ** -0.5, 0.5, ((0, 32),))
    down_weight = bell_draw(key_of[11], (EXPERTS, FF, D), (16 * FF) ** -0.5, 0.0625, ((0, 32),))
    second_gain = jnp.clip(1.0 + 0.18 * jax.random.normal(key_of[12], (D,), jnp.float32), 0.1, 1.9)
    return dict(stream=stream, query_rows=query_rows, key_rows=key_rows, value_rows=value_rows, forget_sums=forget_sums, out_weight=out_weight, first_gain=first_gain, expert_ids=expert_ids, route_scores=route_scores, gate_weight=gate_weight, up_weight=up_weight, down_weight=down_weight, second_gain=second_gain)


deep_alpha = 8.0 ** 0.25
clamp_limit = 7.0
swish_alpha = 1.702
norm_eps = 1e-05
mask_fill = -1e+30

def layer_norm(summed, gain_row):
    centre = lax.optimization_barrier(jnp.mean(summed, axis=-1, keepdims=True))
    spread = lax.optimization_barrier(jnp.mean(jnp.square(summed - centre), axis=-1, keepdims=True))
    return (summed - centre) * lax.rsqrt(spread + norm_eps) * gain_row

def attend_head(query_head, key_head, value_head, gate_head):
    length = query_head.shape[0]
    q_block = min(512, length)
    block_count = length // q_block
    inv_root = query_head.shape[1] ** (-0.5)
    key_pos = jnp.arange(length, dtype=jnp.int32)

    def one_block(block_index):
        first_row = block_index * q_block
        row_block = lax.dynamic_slice_in_dim(query_head, first_row, q_block, 0)
        row_gate = lax.dynamic_slice_in_dim(gate_head, first_row, q_block, 0)
        scores = jnp.dot(row_block, key_head.T, preferred_element_type=jnp.float32) * inv_root
        scores = scores + row_gate[:, None] - gate_head[None, :]
        query_pos = first_row + jnp.arange(q_block, dtype=jnp.int32)
        scores = jnp.where(query_pos[:, None] >= key_pos[None, :], scores, mask_fill)
        row_max = lax.optimization_barrier(jnp.max(scores, axis=1, keepdims=True))
        weights = jnp.exp(scores - row_max)
        row_total = lax.optimization_barrier(jnp.sum(weights, axis=1, keepdims=True))
        blended = jnp.dot(weights.astype(jnp.bfloat16), value_head, preferred_element_type=jnp.float32)
        return (blended / row_total).astype(jnp.bfloat16)
    return lax.map(one_block, jnp.arange(block_count, dtype=jnp.int32)).reshape(length, -1)

def expert_rows(row_block, gate_matrix, up_matrix, down_matrix):
    gate_act = jnp.minimum(jnp.dot(row_block, gate_matrix, preferred_element_type=jnp.float32), clamp_limit)
    up_act = jnp.clip(jnp.dot(row_block, up_matrix, preferred_element_type=jnp.float32), -clamp_limit, clamp_limit)
    hidden = (gate_act * jax.nn.sigmoid(swish_alpha * gate_act) * (up_act + 1.0)).astype(jnp.bfloat16)
    return jnp.dot(hidden, down_matrix, preferred_element_type=jnp.float32).astype(jnp.bfloat16)

def reference(stream, query_rows, key_rows, value_rows, forget_sums, out_weight, first_gain, expert_ids, route_scores, gate_weight, up_weight, down_weight, second_gain):

    def split_heads(head_rows):
        return head_rows.reshape(SEQUENCE_COUNT, SEQUENCE_LENGTH, HEAD_TOTAL, HD).transpose(0, 2, 1, 3).reshape(SEQUENCE_COUNT * HEAD_TOTAL, SEQUENCE_LENGTH, HD)
    attended = lax.map(lambda head_parts: attend_head(head_parts[0], head_parts[1], head_parts[2], head_parts[3]), (split_heads(query_rows), split_heads(key_rows), split_heads(value_rows), forget_sums.reshape(SEQUENCE_COUNT * HEAD_TOTAL, SEQUENCE_LENGTH)))
    attended = attended.reshape(SEQUENCE_COUNT, HEAD_TOTAL, SEQUENCE_LENGTH, HD).transpose(0, 2, 1, 3).reshape(SEQUENCE_COUNT * SEQUENCE_LENGTH, HEAD_TOTAL * HD)
    projected = jnp.dot(attended, out_weight, preferred_element_type=jnp.float32)
    summed = deep_alpha * stream.reshape(SEQUENCE_COUNT * SEQUENCE_LENGTH, D).astype(jnp.float32) + projected
    first_stream = layer_norm(summed, first_gain).astype(jnp.bfloat16)
    flat_ids = expert_ids.reshape(-1).astype(jnp.int32)
    route_weights = jax.nn.softmax(route_scores.reshape(-1, TOP), axis=-1).reshape(-1)
    most_rows = CAP * (SEQUENCE_COUNT * SEQUENCE_LENGTH // TOK_DEV)

    def expert_step(running, inputs):
        gate_matrix, up_matrix, down_matrix, expert_index = inputs
        chosen = flat_ids == expert_index
        picked = jnp.nonzero(chosen, size=most_rows, fill_value=0)[0].astype(jnp.int32)
        is_valid = (jnp.arange(most_rows, dtype=jnp.int32) < jnp.sum(chosen.astype(jnp.int32))).astype(jnp.float32)
        token_index = picked // TOP
        outputs = expert_rows(first_stream[token_index], gate_matrix, up_matrix, down_matrix)
        scaled = outputs.astype(jnp.float32) * (route_weights[picked] * is_valid)[:, None]
        return (running.at[token_index].add(scaled), None)
    mixture, _ = lax.scan(expert_step, jnp.zeros((SEQUENCE_COUNT * SEQUENCE_LENGTH, D), jnp.float32), (gate_weight, up_weight, down_weight, jnp.arange(EXPERTS, dtype=jnp.int32)))
    second = layer_norm(deep_alpha * first_stream.astype(jnp.float32) + mixture, second_gain)
    return second.astype(jnp.bfloat16).reshape(SEQUENCE_COUNT, SEQUENCE_LENGTH, D)
```

```python
import functools

import jax
import jax.numpy as jnp
from jax import lax
from jax.experimental import pallas as pl
from jax.experimental.pallas import tpu as pltpu
from jax.sharding import PartitionSpec as P

deep_alpha = 8.0**0.25
clamp_limit = 7.0
swish_alpha = 1.702
norm_eps = 1e-05
mask_fill = -1e30


def layer_norm(summed, gain_row):
    centre = jnp.mean(summed, axis=-1, keepdims=True)
    spread = jnp.mean(jnp.square(summed - centre), axis=-1, keepdims=True)
    return (summed - centre) * lax.rsqrt(spread + norm_eps) * gain_row


def attend_kernel(
    sp_count, heads, head_size, q_ref, k_ref, v_ref, gate_ref, out_ref,
    q_all, k_all, v_all, blended_all, in_send, in_recv, out_send, out_recv,
):
    me = lax.axis_index("sp")
    rows = q_ref.shape[0]
    length = rows * sp_count
    mesh_id = pl.DeviceIdType.MESH

    def cols(owner, head):
        return pl.ds(pl.multiple_of((owner * heads + head) * head_size, head_size), head_size)

    def band(owner):
        return pl.ds(pl.multiple_of(owner * rows, rows), rows)

    barrier = pltpu.get_barrier_semaphore()
    for step in range(1, sp_count):
        peer = lax.rem(me + step, sp_count)
        pl.semaphore_signal(barrier, inc=1, device_id={"sp": peer}, device_id_type=mesh_id)
    pl.semaphore_wait(barrier, sp_count - 1)

    arrivals = []
    pairs = ((q_ref, q_all), (k_ref, k_all), (v_ref, v_all))
    for head in range(heads):
        copies = []
        for step in range(1, sp_count):
            peer = lax.rem(me + step, sp_count)
            for which, (src, dst) in enumerate(pairs):
                copy = pltpu.make_async_remote_copy(
                    src_ref=src.at[:, cols(peer, head)],
                    dst_ref=dst.at[head, band(me), :],
                    send_sem=in_send.at[head, which, step - 1],
                    recv_sem=in_recv.at[head, which, step - 1],
                    device_id={"sp": peer},
                    device_id_type=mesh_id,
                )
                copy.start()
                copies.append(copy)
        arrivals.append(copies)
    for head in range(heads):
        for src, dst in pairs:
            dst[head, band(me), :] = src[:, cols(me, head)]

    q_block = min(256, length)
    inv_root = head_size ** (-0.5)
    departures = []
    for head in range(heads):
        for copy in arrivals[head]:
            copy.wait_recv()
        for block in range(length // q_block):
            upto = (block + 1) * q_block
            scores = (
                lax.dot_general(
                    q_all[head, block * q_block : upto, :],
                    k_all[head, :upto, :],
                    (((1,), (1,)), ((), ())),
                    preferred_element_type=jnp.float32,
                )
                * inv_root
                - gate_ref[head : head + 1, :upto]
            )
            q_pos = block * q_block + lax.broadcasted_iota(jnp.int32, scores.shape, 0)
            k_pos = lax.broadcasted_iota(jnp.int32, scores.shape, 1)
            scores = jnp.where(q_pos >= k_pos, scores, mask_fill)
            weights = jnp.exp(scores - jnp.max(scores, axis=1, keepdims=True))
            total = jnp.sum(weights, axis=1, keepdims=True)
            blended = jnp.dot(
                weights.astype(jnp.bfloat16),
                v_all[head, :upto, :],
                preferred_element_type=jnp.float32,
            )
            blended_all[head, block * q_block : upto, :] = (blended / total).astype(jnp.bfloat16)
        for step in range(1, sp_count):
            peer = lax.rem(me + step, sp_count)
            copy = pltpu.make_async_remote_copy(
                src_ref=blended_all.at[head, band(peer), :],
                dst_ref=out_ref.at[:, cols(me, head)],
                send_sem=out_send.at[head, step - 1],
                recv_sem=out_recv.at[head, step - 1],
                device_id={"sp": peer},
                device_id_type=mesh_id,
            )
            copy.start()
            departures.append(copy)
        out_ref[:, cols(me, head)] = blended_all[head, band(me), :]
    for copies in arrivals:
        for copy in copies:
            copy.wait_send()
    for copy in departures:
        copy.wait()


def attend(query, key, value, gates, sp_count):
    rows, width = query.shape
    heads, length = gates.shape
    head_size = width // (sp_count * heads)
    whole = pltpu.VMEM((heads, length, head_size), jnp.bfloat16)
    sems = pltpu.SemaphoreType.DMA
    return pl.pallas_call(
        functools.partial(attend_kernel, sp_count, heads, head_size),
        out_shape=jax.ShapeDtypeStruct((rows, width), jnp.bfloat16),
        in_specs=[pl.BlockSpec(memory_space=pltpu.VMEM)] * 4,
        out_specs=pl.BlockSpec(memory_space=pltpu.VMEM),
        scratch_shapes=[
            whole, whole, whole, whole,
            sems((heads, 3, sp_count - 1)),
            sems((heads, 3, sp_count - 1)),
            sems((heads, sp_count - 1)),
            sems((heads, sp_count - 1)),
        ],
        compiler_params=pltpu.CompilerParams(
            collective_id=0, has_side_effects=True, vmem_limit_bytes=40 * 2**20
        ),
        name="attend",
    )(query, key, value, gates)


def expert_rows(row_block, gate_matrix, up_matrix, down_matrix):
    gate_act = jnp.minimum(
        jnp.dot(row_block, gate_matrix, preferred_element_type=jnp.float32), clamp_limit
    )
    up_act = jnp.clip(
        jnp.dot(row_block, up_matrix, preferred_element_type=jnp.float32), -clamp_limit, clamp_limit
    )
    hidden = (gate_act * jax.nn.sigmoid(swish_alpha * gate_act) * (up_act + 1.0)).astype(
        jnp.bfloat16
    )
    return jnp.dot(hidden, down_matrix, preferred_element_type=jnp.float32).astype(jnp.bfloat16)


def shards(
    stream,
    query_rows,
    key_rows,
    value_rows,
    forget_sums,
    out_weight,
    first_gain,
    expert_ids,
    route_scores,
    gate_weight,
    up_weight,
    down_weight,
    second_gain,
):
    attended = attend(
        query_rows[0], key_rows[0], value_rows[0], forget_sums[0], lax.axis_size("sp")
    )
    projected = jnp.dot(attended, out_weight, preferred_element_type=jnp.float32)
    first_stream = layer_norm(
        deep_alpha * stream[0].astype(jnp.float32) + projected, first_gain
    ).astype(jnp.bfloat16)
    tokens_here = expert_ids.shape[1]
    top_k = expert_ids.shape[2]
    model_width = first_stream.shape[1]
    sp_count = lax.axis_size("sp")
    dp_count = lax.axis_size("dp")
    expert_count = sp_count * dp_count
    capacity = max(2, 3 * tokens_here * top_k // (2 * expert_count))
    flat_ids = expert_ids[0].reshape(-1)
    one_hot = (flat_ids[:, None] == jnp.arange(expert_count, dtype=jnp.int32)[None, :]).astype(
        jnp.int32
    )
    slot_ids = jnp.sum((jnp.cumsum(one_hot, axis=0) - one_hot) * one_hot, axis=1)
    slot_index = flat_ids * capacity + slot_ids
    slot_range = jnp.arange(expert_count * capacity, dtype=jnp.int32)
    matches = slot_range[:, None] == slot_index[None, :]
    dispatch = jnp.sum(matches.astype(jnp.int32).reshape(-1, tokens_here, top_k), axis=2).astype(
        jnp.bfloat16
    )
    outgoing = jnp.dot(dispatch, first_stream, preferred_element_type=jnp.float32).astype(
        jnp.bfloat16
    )
    outgoing = outgoing.reshape(expert_count, capacity, model_width)
    arrived = lax.all_to_all(outgoing, ("sp", "dp"), split_axis=0, concat_axis=0, tiled=True)
    finished = expert_rows(
        arrived.reshape(-1, model_width), gate_weight[0], up_weight[0], down_weight[0]
    )
    returned = lax.all_to_all(
        finished.reshape(arrived.shape), ("sp", "dp"), split_axis=0, concat_axis=0, tiled=True
    )
    route_weights = jax.nn.softmax(route_scores[0], axis=-1).reshape(-1)
    combine = jnp.sum(
        jnp.where(matches, route_weights[None, :], 0.0).reshape(-1, tokens_here, top_k), axis=2
    )
    mixture = lax.dot_general(
        combine,
        returned.reshape(-1, model_width).astype(jnp.float32),
        (((0,), (0,)), ((), ())),
        precision=lax.Precision.HIGHEST,
        preferred_element_type=jnp.float32,
    )
    second = layer_norm(deep_alpha * first_stream.astype(jnp.float32) + mixture, second_gain)
    return second.astype(jnp.bfloat16)[None]


def solution(mesh):
    return jax.shard_map(
        shards,
        mesh=mesh,
        in_specs=(
            P("dp", "sp", None),
            P("dp", "sp", None),
            P("dp", "sp", None),
            P("dp", "sp", None),
            P("dp", "sp", None),
            P(),
            P(),
            P("dp", "sp", None),
            P("dp", "sp", None),
            P(("sp", "dp"), None, None),
            P(("sp", "dp"), None, None),
            P(("sp", "dp"), None, None),
            P(),
        ),
        out_specs=P("dp", "sp", None),
        check_vma=False,
    )
```
